512 devices in a mesh: fs: 64 (over z, y), rep: 4 (over x), tp: 2 (over core).
Axes of the slice: x: 4, y: 8, z: 8, core: 2. Of those that a mesh axis runs over, the one named last changes fastest.
Arguments:
- tokens_in: bfloat16 [131072, 2048], P(('fs', 'rep')), may hold values from -24 to 24
- query_two: bfloat16 [131072, 512], P(('fs', 'rep'), 'tp'), may hold values from -49 to 49
- key_two: bfloat16 [131072, 512], P(('fs', 'rep'), 'tp'), may hold values from -9 to 9
- values: bfloat16 [131072, 1024], P(('fs', 'rep'), 'tp'), may hold values from -6 to 6
- out_grad: bfloat16 [131072, 1024], P(('fs', 'rep'), 'tp'), may hold values from -6 to 6
- second_scale: float32 [8], P('tp'), may hold values from 0.3 to 0.8
- factor: bfloat16 [2048, 256], P('fs'), may hold values from -0.125 to 0.125
- weight: float32 [2048, 512], P('fs', 'tp'), may hold values from -0.6 to 0.6
- first_moment: float32 [256, 512], P('fs', 'tp'), may hold values from -543.058 to 543.058
- second_moment: float32 [256, 512], P('fs', 'tp'), may hold values from 81 to 131072
Outputs:
- new_weight: float32 [2048, 512], P('fs', 'tp')
- weight_copy: bfloat16 [2048, 512], P(None, 'tp')
- update_step: float32 [2048, 512], P('fs', 'tp')
- new_first: float32 [256, 512], P('fs', 'tp')
- new_second: float32 [256, 512], P('fs', 'tp')
The draws below stay inside these ranges and needn't reach their ends.
All inputs are finite; a program needn't handle non-finite values.
Results may differ from the reference program's by a relative error of at most 0.006.
Values may be sent and summed in bfloat16 or wider, within the bound.
No kernel may reach another device: no remote copies, remote signals or barrier semaphores. Data moves between devices by JAX's collectives and lax.ppermute only.
A program may use at most 64 MiB of HBM per device.

```python
import jax
import jax.numpy as jnp
from jax import lax

D = 2048
HEADS_W = 8
VD = 128
RANK = 256
TOK_DEV = 512
KW = 512
TOKENS = 131072


def drawn_pair(key):
    base = jax.random.fold_in(key, 11)
    key_query, key_keys = jax.random.split(base, 2)
    queries = jnp.clip(1.4 * jax.random.normal(key_query, (TOKENS, KW), jnp.float32), -8.4, 8.4)
    keys_all = jnp.clip(1.4 * jax.random.normal(key_keys, (TOKENS, KW), jnp.float32), -8.4, 8.4)
    return (queries, keys_all)


def draw_query_two(key, part):
    return drawn_pair(key)[0].astype(jnp.bfloat16)


def draw_key_two(key, part):
    return drawn_pair(key)[1].astype(jnp.bfloat16)


def draw_first_moment(key, part):
    base = jax.random.fold_in(key, 23)
    moment_scale = 0.25 * TOKENS ** 0.5
    raw_values = jnp.clip(jax.random.normal(base, (RANK, KW), jnp.float32), -6.0, 6.0)
    return moment_scale * raw_values


def draw_second_moment(key, part):
    base = jax.random.fold_in(key, 37)
    rank_index = jnp.arange(RANK, dtype=jnp.float32)[:, None]
    falling = 100.0 ** (-rank_index / max(RANK - 1, 1))
    jitter = jnp.exp(jax.random.uniform(base, (RANK, KW), jnp.float32, -0.693, 0.693))
    return 0.25 * TOKENS * falling * jitter


def with_spikes(values, rng, source, target, shards_of, factor):
    owner, partner = [(jnp.arange(values.shape[dim]) // (values.shape[dim] // shards_of)).reshape([-1 if axis == dim else 1 for axis in range(values.ndim)]) for dim in (source, target)]
    chosen = jax.random.permutation(rng, shards_of)[partner]
    strong = (owner == chosen) | (owner == (partner + shards_of // 2) % shards_of)
    return jnp.where(strong, factor * values, values)


def block_levels(own_key, dims, cuts, least, top_value):
    gain, own = 1.0, jax.random.fold_in(own_key, 6)
    for dim, shards_of in cuts:
        draws = jnp.exp(jax.random.uniform(jax.random.fold_in(own, dim), (shards_of,), jnp.float32, least / len(cuts), top_value / len(cuts)))
        gain = gain * jnp.repeat(draws, dims[dim] // shards_of).reshape([-1 if axis == dim else 1 for axis in range(len(dims))])
    return gain


def noise(key, extent, width, most, cuts=(), kind=jnp.bfloat16):
    array = jax.random.normal(key, extent, jnp.float32) * width
    if len(cuts) > 0:
        array = block_levels(key, extent, cuts, -0.22, 0.18) * array
    return jnp.clip(array, min=-most, max=most).astype(kind)


def heavy_noise(own_key, shape, spread, most, cuts, heavy, held_as=jnp.bfloat16):
    values = spread * jax.random.normal(own_key, shape, jnp.float32)
    if cuts:
        values = values * block_levels(own_key, shape, cuts, -0.22, 0.18)
    return jnp.clip(with_spikes(values, jax.random.fold_in(own_key, 3), *heavy), -most, most).astype(held_as)


def setup_inputs(seed: int = 0) -> dict:
    keys = jax.random.split(jax.random.key(seed), 11)
    return {
        "tokens_in": heavy_noise(keys[0], (TOKENS, D), 1.0, 24.0, ((0, 256),), (0, 1, 256, 6.0)),
        "query_two": draw_query_two(jax.random.fold_in(keys[10], 71), 0),
        "key_two": draw_key_two(jax.random.fold_in(keys[10], 71), 0),
        "values": noise(keys[3], (TOKENS, HEADS_W * VD), 1.0, 6.0, ((0, 256), (1, 2))),
        "out_grad": noise(keys[4], (TOKENS, HEADS_W * VD), 1.0, 6.0, ((0, 256), (1, 2))),
        "second_scale": jnp.clip(0.3 + 0.5 * jax.random.uniform(keys[5], (HEADS_W,), jnp.float32) ** block_levels(keys[5], (HEADS_W,), ((0, 2),), -0.2, 0.2), 0.3, 0.8),
        "factor": noise(keys[6], (D, RANK), D ** -0.5, 0.125, ((0, 64),)),
        "weight": noise(keys[7], (D, KW), 0.1, 0.6, ((0, 64), (1, 2)), jnp.float32),
        "first_moment": draw_first_moment(jax.random.fold_in(keys[10], 71), 0),
        "second_moment": draw_second_moment(jax.random.fold_in(keys[10], 71), 0),
    }


def key_gradient(query_rows, key_rows, value_rows, grad_rows, second_scale):
    length = query_rows.shape[0]
    head_count = second_scale.shape[0]
    queries = query_rows.astype(jnp.float32).reshape(length, head_count, -1)
    keys_all = key_rows.astype(jnp.float32).reshape(length, head_count, -1)
    value_heads = value_rows.astype(jnp.float32).reshape(length, head_count, -1)
    grad_heads = grad_rows.astype(jnp.float32).reshape(length, head_count, -1)
    inv_root = queries.shape[2] ** (-0.5)
    scores = jnp.einsum('qhd,khd->hqk', queries, keys_all) * inv_root
    positions = jnp.arange(length, dtype=jnp.int32)
    causal = positions[:, None] >= positions[None, :]
    scores = jnp.where(causal[None], scores, -1e+30)
    row_peak = lax.optimization_barrier(jnp.max(scores, axis=-1, keepdims=True))
    exps = jnp.exp(scores - row_peak)
    weights_map = exps / lax.optimization_barrier(jnp.sum(exps, axis=-1, keepdims=True))
    attn_grad = jnp.einsum('qhe,khe->hqk', grad_heads, value_heads)
    row_inner = lax.optimization_barrier(jnp.sum(weights_map * attn_grad, axis=-1, keepdims=True))
    score_grad = ((-second_scale)[:, None, None] * weights_map * (attn_grad - row_inner)).astype(jnp.bfloat16)
    score_grad = lax.optimization_barrier(score_grad)
    key_grad = jnp.einsum('hqk,qhd->khd', score_grad.astype(jnp.float32), queries) * inv_root
    return key_grad.reshape(length, -1).astype(jnp.bfloat16)

def reference(tokens_in, query_two, key_two, values, out_grad, second_scale, factor, weight, first_moment, second_moment):
    sequences = TOKENS // TOK_DEV

    def accumulate(running, pieces):
        token_rows, query_rows, key_rows, value_rows, grad_rows = pieces
        key_grad = key_gradient(query_rows, key_rows, value_rows, grad_rows, second_scale)
        return (running + jnp.dot(token_rows.T, key_grad, preferred_element_type=jnp.float32), None)
    pieces = (tokens_in.reshape(sequences, TOK_DEV, D), query_two.reshape(sequences, TOK_DEV, KW), key_two.reshape(sequences, TOK_DEV, KW), values.reshape(sequences, TOK_DEV, HEADS_W * VD), out_grad.reshape(sequences, TOK_DEV, HEADS_W * VD))
    gradient, unused_out = lax.scan(accumulate, jnp.zeros((D, KW), jnp.float32), pieces)
    projected = jnp.dot(factor.astype(jnp.float32).T, gradient, precision=lax.Precision.HIGHEST)
    new_first = 0.9 * first_moment + 0.1 * projected
    new_second = 0.95 * second_moment + 0.05 * projected * projected
    direction = (new_first / (jnp.sqrt(new_second) + 1e-08)).astype(jnp.bfloat16)
    squares = jnp.sum(jnp.square(lax.optimization_barrier(direction).astype(jnp.float32)))
    update_step = jnp.dot(factor, direction, preferred_element_type=jnp.float32) * lax.rsqrt(squares / (RANK * KW) + 1e-06)
    new_weight = weight - 0.1 * update_step
    return (new_weight, new_weight.astype(jnp.bfloat16), update_step, new_first, new_second)
```

```python
import jax
import jax.numpy as jnp
from jax import lax
from jax.sharding import PartitionSpec as P


RANK = 256
KW = 512
BF16 = jnp.bfloat16
F32 = jnp.float32

by_rows = (((0,), (0,)), ((), ()))


def dot32(left, right):
    return jnp.dot(left, right, preferred_element_type=F32)


def sent_to_all(value, axis, count):
    return lax.all_to_all(
        jnp.broadcast_to(value[None], (count, *value.shape)), axis, 0, 0, tiled=True
    )


def to_bf16(value):
    return lax.reduce_precision(value, exponent_bits=8, mantissa_bits=7)


def parts_of(value):
    high = to_bf16(value)
    middle = to_bf16(value - high)
    low = to_bf16(value - high - middle)
    return high.astype(BF16), middle.astype(BF16), low.astype(BF16)


def key_gradient(query_rows, key_rows, value_rows, grad_rows, second_scale):
    length = query_rows.shape[0]
    head_count = second_scale.shape[0]
    queries = query_rows.reshape(length, head_count, -1)
    keys_all = key_rows.reshape(length, head_count, -1)
    value_heads = value_rows.reshape(length, head_count, -1)
    grad_heads = grad_rows.reshape(length, head_count, -1)
    inv_root = queries.shape[2] ** (-0.5)
    scores = (
        jnp.einsum("qhd,khd->hqk", queries, keys_all, preferred_element_type=jnp.float32) * inv_root
    )
    positions = jnp.arange(length, dtype=jnp.int32)
    causal = positions[:, None] >= positions[None, :]
    scores = jnp.where(causal[None], scores, -1e30)
    row_peak = jnp.max(scores, axis=-1, keepdims=True)
    exps = jnp.exp(scores - row_peak)
    weights_map = exps / jnp.sum(exps, axis=-1, keepdims=True)
    attn_grad = jnp.einsum(
        "qhe,khe->hqk", grad_heads, value_heads, preferred_element_type=jnp.float32
    )
    row_inner = jnp.sum(weights_map * attn_grad, axis=-1, keepdims=True)
    score_grad = ((-second_scale)[:, None, None] * weights_map * (attn_grad - row_inner)).astype(
        jnp.bfloat16
    )
    key_grad = (
        jnp.einsum("hqk,qhd->khd", score_grad, queries, preferred_element_type=jnp.float32)
        * inv_root
    )
    return key_grad.reshape(length, -1).astype(jnp.bfloat16)


def on_device(
    tokens_in,
    query_two,
    key_two,
    values,
    out_grad,
    second_scale,
    factor,
    weight,
    first_moment,
    second_moment,
):
    shards = lax.axis_size("fs")
    reps = lax.axis_size("rep")
    core = lax.axis_index("tp")
    rank = factor.shape[1]
    half = rank // 2
    own_rows = first_moment.shape[0]
    pairs = own_rows // 2
    rows_here, cols = weight.shape

    ranks = lax.broadcasted_iota(jnp.int32, (rank, half), 0)
    places = lax.broadcasted_iota(jnp.int32, (rank, half), 1)
    mine = dot32(factor, (ranks == 2 * places + core).astype(BF16)).astype(BF16)
    other = dot32(factor, (ranks == 2 * places + 1 - core).astype(BF16)).astype(BF16)

    share = rows_here // reps
    rep = lax.axis_index("rep")
    old_share = lax.dynamic_slice_in_dim(weight, rep * share, share, 0).astype(BF16)
    old_share = jnp.concatenate([old_share[:, i : i + half] for i in range(0, cols, half)], axis=0)
    first_sent = sent_to_all(jnp.concatenate([mine, old_share], axis=0), "fs", shards)
    factor_mine = first_sent[:, :rows_here].reshape(-1, half)
    old_mine = first_sent[:, rows_here:]

    moments = lax.all_gather(jnp.concatenate([first_moment, second_moment], 0), "tp")
    moments = jnp.concatenate([moments[0], moments[1]], axis=1)
    first_both, second_both = moments[:own_rows], moments[own_rows:]

    key_grad = key_gradient(query_two, key_two, values, out_grad, second_scale)
    key_both = lax.all_gather(key_grad, "tp")

    reduced = dot32(tokens_in, factor_mine)
    reduced_high = reduced.astype(BF16)
    reduced_low = (reduced - reduced_high.astype(F32)).astype(BF16)
    sums = [
        lax.dot_general(reduced_high, key_both[i], by_rows, preferred_element_type=F32)
        + lax.dot_general(reduced_low, key_both[i], by_rows, preferred_element_type=F32)
        for i in range(2)
    ]
    sums = jnp.concatenate(sums, axis=1).astype(BF16)

    arrived = lax.all_to_all(sums.reshape(shards, pairs, 2 * cols), "fs", 0, 0, tiled=True)
    factor_other = lax.ppermute(factor_mine, "tp", [(0, 1), (1, 0)])
    factor_all = jnp.concatenate([factor_mine, factor_other], axis=1)
    own_factor = jnp.concatenate([mine, other], axis=1)
    old_all = jnp.zeros((shards, reps, *old_mine.shape[1:]), BF16)
    old_all = lax.dynamic_update_index_in_dim(old_all, old_mine, rep, 1)
    for i in range(1, reps):
        came = lax.ppermute(old_mine, "rep", [(j, (j + i) % reps) for j in range(reps)])
        old_all = lax.dynamic_update_index_in_dim(old_all, came, (rep + reps - i) % reps, 1)
    old_all = old_all.reshape(shards, reps, cols // half, share, half)
    old_weight = jnp.moveaxis(old_all, 2, 3).reshape(-1, cols)

    part = jnp.sum(arrived.astype(F32), axis=0)
    part = sent_to_all(part, ("rep", "tp"), 2 * reps)
    part = part.reshape(reps, 2, pairs, 2 * cols).sum(axis=0)
    projected = jnp.stack([part[0], part[1]], axis=1).reshape(own_rows, 2 * cols)

    new_first = 0.9 * first_both + 0.1 * projected
    new_second = 0.95 * second_both + 0.05 * projected * projected
    direction = (new_first / (jnp.sqrt(new_second) + 1e-08)).astype(BF16)
    own_squares = jnp.sum(jnp.square(direction.astype(F32)))

    def own_cols(value):
        return jnp.where(core == 0, value[:, :cols], value[:, cols:])

    own_direction = own_cols(direction).reshape(pairs, 2 * cols)
    high, middle, low = parts_of(own_squares)
    lane = lax.broadcasted_iota(jnp.int32, (pairs, 128), 1)
    row = lax.broadcasted_iota(jnp.int32, (pairs, 128), 0)
    zero = jnp.zeros((), BF16)
    packed = jnp.where(lane == 0, high, jnp.where(lane == 1, middle, jnp.where(lane == 2, low, zero)))
    packed = jnp.where(row == 0, packed, zero)
    gathered = sent_to_all(jnp.concatenate([own_direction, packed], axis=1), "fs", shards)
    squares = jnp.sum(gathered[:, :, 2 * cols :].astype(F32))
    even = gathered[:, :, :cols].reshape(-1, cols)
    odd = gathered[:, :, cols : 2 * cols].reshape(-1, cols)
    rows = jnp.concatenate(
        [jnp.where(core == 0, even, odd), jnp.where(core == 0, odd, even)], axis=0
    )

    rate = lax.rsqrt(squares / (RANK * KW) + 1e-06)
    update_step = dot32(own_factor, rows) * rate
    new_weight = weight - 0.1 * update_step
    copies = (old_weight.astype(F32) - 0.1 * (dot32(factor_all, rows) * rate)).astype(BF16)
    return (new_weight, copies, update_step, own_cols(new_first), own_cols(new_second))


def solution(mesh):
    in_specs = (
        P(("fs", "rep"), None),
        P(("fs", "rep"), "tp"),
        P(("fs", "rep"), "tp"),
        P(("fs", "rep"), "tp"),
        P(("fs", "rep"), "tp"),
        P("tp"),
        P("fs", None),
        P("fs", "tp"),
        P("fs", "tp"),
        P("fs", "tp"),
    )
    out_specs = (P("fs", "tp"), P(None, "tp"), P("fs", "tp"), P("fs", "tp"), P("fs", "tp"))

    return jax.shard_map(
        on_device, mesh=mesh, in_specs=in_specs, out_specs=out_specs, check_vma=False
    )
```

```python
import jax
import jax.numpy as jnp
from jax import lax
from jax.experimental import pallas as pl
from jax.experimental.pallas import tpu as pltpu
from jax.sharding import PartitionSpec as P


RANK = 256
KW = 512
BF16 = jnp.bfloat16
F32 = jnp.float32


def dot32(left, right):
    return jnp.dot(left, right, preferred_element_type=F32)


def sent_to_all(value, axis, count):
    return lax.all_to_all(
        jnp.broadcast_to(value[None], (count, *value.shape)), axis, 0, 0, tiled=True
    )


def dot_rows(left, right):
    return lax.dot_general(left, right, (((1,), (1,)), ((), ())), preferred_element_type=F32)


def key_gradient_body(scale_ref, query_ref, key_ref, value_ref, grad_ref, out_ref):
    length = query_ref.shape[0]
    block = length // 2
    heads = scale_ref.shape[0]
    dim = query_ref.shape[1] // heads
    wide = value_ref.shape[1] // heads
    inv_root = dim ** (-0.5)
    pair = 2 * dim
    lane = lax.broadcasted_iota(jnp.int32, (block, pair), 1)
    later = lax.broadcasted_iota(jnp.int32, (block, block), 0) > lax.broadcasted_iota(
        jnp.int32, (block, block), 1
    )
    for first in range(0, heads, 2):
        lanes = slice(first * dim, first * dim + pair)
        found = [[], []]
        for side in range(2):
            head = first + side
            span = slice(head * wide, head * wide + wide)
            for step in range(2):
                rows = slice(step * block, step * block + block)
                seen = block * (step + 1)
                own = query_ref[rows, lanes].astype(F32) * inv_root
                own = jnp.where((lane >= dim) == (side == 1), own, 0.0).astype(BF16)
                scores = dot_rows(key_ref[:seen, lanes], own)
                last = jnp.where(later, -1e30, scores[seen - block :])
                scores = jnp.concatenate([scores[: seen - block], last], axis=0) if step else last
                exps = jnp.exp(scores - jnp.max(scores, axis=0, keepdims=True))
                total = jnp.sum(exps, axis=0, keepdims=True)
                attn_grad = dot_rows(value_ref[:seen, span], grad_ref[rows, span])
                weights_map = exps / total
                inner = jnp.sum(weights_map * attn_grad, axis=0, keepdims=True)
                score_grad = (-scale_ref[head] * weights_map * (attn_grad - inner)).astype(BF16)
                for place in range(step + 1):
                    found[place].append(
                        dot32(score_grad[place * block : place * block + block], own)
                    )
        for place in range(2):
            total = found[place][0]
            for more in found[place][1:]:
                total = total + more
            out_ref[place * block : place * block + block, lanes] = total.astype(BF16)


def key_gradient(query_rows, key_rows, value_rows, grad_rows, second_scale):
    return pl.pallas_call(
        key_gradient_body,
        out_shape=jax.ShapeDtypeStruct(query_rows.shape, BF16),
        in_specs=[pl.BlockSpec(memory_space=pltpu.SMEM)] + 4 * [pl.BlockSpec(memory_space=pltpu.VMEM)],
        out_specs=pl.BlockSpec(memory_space=pltpu.VMEM),
        name="key_gradient",
    )(second_scale, query_rows, key_rows, value_rows, grad_rows)


def first_message_body(place_ref, factor_ref, weight_ref, out_ref, own_ref):
    shards = out_ref.shape[0]
    rows, rank = factor_ref.shape
    half = rank // 2
    share = (out_ref.shape[1] - rows) // 2
    core = place_ref[0]
    ranks = lax.broadcasted_iota(jnp.int32, (rank, half), 0)
    places = lax.broadcasted_iota(jnp.int32, (rank, half), 1)
    factor = factor_ref[...]
    mine = dot32(factor, (ranks == 2 * places + core).astype(F32).astype(BF16)).astype(BF16)
    other = dot32(factor, (ranks == 2 * places + 1 - core).astype(F32).astype(BF16)).astype(BF16)
    own_ref[:, :half] = mine
    own_ref[:, half:] = other
    old = weight_ref[pl.ds(pl.multiple_of(place_ref[1] * share, share), share), :].astype(BF16)
    out_ref[:, :rows, :] = jnp.broadcast_to(mine[None], (shards, rows, half))
    for i in range(2):
        piece = old[:, i * half : i * half + half]
        out_ref[:, rows + i * share : rows + i * share + share, :] = jnp.broadcast_to(
            piece[None], (shards, share, half)
        )


def first_message(places, factor, weight, shards, reps):
    rows, rank = factor.shape
    half = rank // 2
    return pl.pallas_call(
        first_message_body,
        out_shape=(
            jax.ShapeDtypeStruct((shards, rows + 2 * (rows // reps), half), BF16),
            jax.ShapeDtypeStruct((rows, rank), BF16),
        ),
        in_specs=[pl.BlockSpec(memory_space=pltpu.SMEM)] + 2 * [pl.BlockSpec(memory_space=pltpu.VMEM)],
        out_specs=2 * (pl.BlockSpec(memory_space=pltpu.VMEM),),
        name="first_message",
    )(places, factor, weight)


def projected_sums_body(tokens_ref, factor_ref, grad_ref, out_ref):
    cols = grad_ref.shape[2]
    reduced = dot32(tokens_ref[...], factor_ref[...]).T
    high = reduced.astype(BF16)
    low = (reduced - high.astype(F32)).astype(BF16)
    for i in range(2):
        grads = grad_ref[i]
        out_ref[:, i * cols : i * cols + cols] = (dot32(high, grads) + dot32(low, grads)).astype(BF16)


def projected_sums(tokens, factor, grads):
    half = factor.shape[1]
    return pl.pallas_call(
        projected_sums_body,
        out_shape=jax.ShapeDtypeStruct((half, 2 * grads.shape[2]), BF16),
        in_specs=3 * [pl.BlockSpec(memory_space=pltpu.VMEM)],
        out_specs=pl.BlockSpec(memory_space=pltpu.VMEM),
        name="projected_sums",
    )(tokens, factor, grads)


def moments_step_body(place_ref, part_ref, moments_ref, message_ref, first_ref, second_ref):
    own_rows, cols = first_ref.shape
    pairs = own_rows // 2
    core = place_ref[0]
    part = part_ref[...]
    total = part[:own_rows]
    for i in range(own_rows, part.shape[0], own_rows):
        total = total + part[i : i + own_rows]
    order = [parity * pairs + place for place in range(pairs) for parity in range(2)]
    projected = jnp.concatenate([total[i : i + 1] for i in order], axis=0)
    both = [
        jnp.concatenate([moments_ref[0, rows, :], moments_ref[1, rows, :]], axis=1)
        for rows in (slice(0, own_rows), slice(own_rows, 2 * own_rows))
    ]
    new_first = 0.9 * both[0] + 0.1 * projected
    new_second = 0.95 * both[1] + 0.05 * projected * projected
    direction = (new_first / (jnp.sqrt(new_second) + 1e-08)).astype(BF16).astype(F32)
    squares = direction * direction
    squares = jnp.sum(jnp.sum(squares, axis=1, keepdims=True), axis=0, keepdims=True)

    def own_cols(value):
        return jnp.where(core == 0, value[:, :cols], value[:, cols:])

    first_ref[...] = own_cols(new_first)
    second_ref[...] = own_cols(new_second)
    own = own_cols(direction)
    for place in range(pairs):
        for parity in range(2):
            row = 2 * place + parity
            message_ref[place : place + 1, parity * cols : parity * cols + cols] = own[row : row + 1]
    high = squares.astype(BF16).astype(F32)
    middle = (squares - high).astype(BF16).astype(F32)
    low = squares - high - middle
    lane = lax.broadcasted_iota(jnp.int32, (pairs, 128), 1)
    row = lax.broadcasted_iota(jnp.int32, (pairs, 128), 0)
    packed = jnp.where(lane == 0, high, jnp.where(lane == 1, middle, jnp.where(lane == 2, low, 0.0)))
    message_ref[:, 2 * cols :] = jnp.where(row == 0, packed, 0.0)


def moments_step(places, part, moments):
    own_rows = moments.shape[1] // 2
    cols = moments.shape[2]
    return pl.pallas_call(
        moments_step_body,
        out_shape=(
            jax.ShapeDtypeStruct((own_rows // 2, 2 * cols + 128), F32),
            jax.ShapeDtypeStruct((own_rows, cols), F32),
            jax.ShapeDtypeStruct((own_rows, cols), F32),
        ),
        in_specs=[pl.BlockSpec(memory_space=pltpu.SMEM)] + 2 * [pl.BlockSpec(memory_space=pltpu.VMEM)],
        out_specs=3 * (pl.BlockSpec(memory_space=pltpu.VMEM),),
        name="moments_step",
    )(places, part, moments)


def on_device(
    tokens_in,
    query_two,
    key_two,
    values,
    out_grad,
    second_scale,
    factor,
    weight,
    first_moment,
    second_moment,
):
    shards = lax.axis_size("fs")
    reps = lax.axis_size("rep")
    core = lax.axis_index("tp")
    rank = factor.shape[1]
    half = rank // 2
    own_rows = first_moment.shape[0]
    pairs = own_rows // 2
    rows_here, cols = weight.shape

    places = jnp.stack([core, lax.axis_index("rep")])
    message, own_factor = first_message(places, factor, weight, shards, reps)
    share = rows_here // reps
    rep = lax.axis_index("rep")
    first_sent = lax.all_to_all(message, "fs", 0, 0, tiled=True)
    factor_mine = first_sent[:, :rows_here].reshape(-1, half)
    old_mine = first_sent[:, rows_here:]

    moments = lax.all_gather(jnp.concatenate([first_moment, second_moment], 0), "tp")
    moments = moments.reshape(2, 2 * own_rows, cols)

    key_grad = key_gradient(query_two, key_two, values, out_grad, second_scale)
    key_both = lax.all_gather(key_grad, "tp")

    sums = projected_sums(tokens_in, factor_mine, key_both)

    arrived = lax.all_to_all(sums.reshape(shards, pairs, 2 * cols), "fs", 0, 0, tiled=True)
    factor_other = lax.ppermute(factor_mine, "tp", [(0, 1), (1, 0)])
    factor_all = jnp.concatenate([factor_mine, factor_other], axis=1)
    old_all = jnp.zeros((shards, reps, *old_mine.shape[1:]), BF16)
    old_all = lax.dynamic_update_index_in_dim(old_all, old_mine, rep, 1)
    for i in range(1, reps):
        came = lax.ppermute(old_mine, "rep", [(j, (j + i) % reps) for j in range(reps)])
        old_all = lax.dynamic_update_index_in_dim(old_all, came, (rep + reps - i) % reps, 1)
    old_all = old_all.reshape(shards, reps, cols // half, share, half)
    old_weight = jnp.moveaxis(old_all, 2, 3).reshape(-1, cols)

    part = jnp.sum(arrived.astype(F32), axis=0)
    part = sent_to_all(part, ("rep", "tp"), 2 * reps)
    message, new_first, new_second = moments_step(
        places, part.reshape(reps * own_rows, 2 * cols), moments
    )
    gathered = sent_to_all(message.astype(BF16), "fs", shards)
    squares = jnp.sum(gathered[:, :, 2 * cols :].astype(F32))
    even = gathered[:, :, :cols].reshape(-1, cols)
    odd = gathered[:, :, cols : 2 * cols].reshape(-1, cols)
    rows = jnp.concatenate(
        [jnp.where(core == 0, even, odd), jnp.where(core == 0, odd, even)], axis=0
    )

    rate = lax.rsqrt(squares / (RANK * KW) + 1e-06)
    update_step = dot32(own_factor, rows) * rate
    new_weight = weight - 0.1 * update_step
    copies = (old_weight.astype(F32) - 0.1 * (dot32(factor_all, rows) * rate)).astype(BF16)
    return (new_weight, copies, update_step, new_first, new_second)


def solution(mesh):
    in_specs = (
        P(("fs", "rep"), None),
        P(("fs", "rep"), "tp"),
        P(("fs", "rep"), "tp"),
        P(("fs", "rep"), "tp"),
        P(("fs", "rep"), "tp"),
        P("tp"),
        P("fs", None),
        P("fs", "tp"),
        P("fs", "tp"),
        P("fs", "tp"),
    )
    out_specs = (P("fs", "tp"), P(None, "tp"), P("fs", "tp"), P("fs", "tp"), P("fs", "tp"))

    return jax.shard_map(on_device, mesh=mesh, in_specs=in_specs, out_specs=out_specs, check_vma=False)
```

```python
import jax
import jax.numpy as jnp
from jax import lax
from jax.experimental import pallas as pl
from jax.experimental.pallas import tpu as pltpu
from jax.sharding import PartitionSpec as P


RANK = 256
KW = 512
BF16 = jnp.bfloat16
F32 = jnp.float32

MIB = 1024 * 1024
VMEM_SPEC = pl.BlockSpec(memory_space=pltpu.VMEM)


def dot32(left, right):
    return jnp.dot(left, right, preferred_element_type=F32)


def dot_rows(left, right):
    return lax.dot_general(left, right, (((1,), (1,)), ((), ())), preferred_element_type=F32)


def key_gradient_body(scale_ref, query_ref, key_ref, value_ref, grad_ref, out_ref):
    length = query_ref.shape[0]
    block = length // 2
    heads = scale_ref.shape[0]
    dim = query_ref.shape[1] // heads
    wide = value_ref.shape[1] // heads
    inv_root = dim ** (-0.5)
    pair = 2 * dim
    lane = lax.broadcasted_iota(jnp.int32, (block, pair), 1)
    later = lax.broadcasted_iota(jnp.int32, (block, block), 0) > lax.broadcasted_iota(
        jnp.int32, (block, block), 1
    )
    for first in range(0, heads, 2):
        lanes = slice(first * dim, first * dim + pair)
        found = [[], []]
        for side in range(2):
            head = first + side
            span = slice(head * wide, head * wide + wide)
            for step in range(2):
                rows = slice(step * block, step * block + block)
                seen = block * (step + 1)
                own = query_ref[rows, lanes].astype(F32) * inv_root
                own = jnp.where((lane >= dim) == (side == 1), own, 0.0).astype(BF16)
                scores = dot_rows(key_ref[:seen, lanes], own)
                last = jnp.where(later, -1e30, scores[seen - block :])
                scores = jnp.concatenate([scores[: seen - block], last], axis=0) if step else last
                exps = jnp.exp(scores - jnp.max(scores, axis=0, keepdims=True))
                total = jnp.sum(exps, axis=0, keepdims=True)
                attn_grad = dot_rows(value_ref[:seen, span], grad_ref[rows, span])
                weights_map = exps / total
                inner = jnp.sum(weights_map * attn_grad, axis=0, keepdims=True)
                score_grad = (-scale_ref[head] * weights_map * (attn_grad - inner)).astype(BF16)
                for place in range(step + 1):
                    found[place].append(
                        dot32(score_grad[place * block : place * block + block], own)
                    )
        for place in range(2):
            total = found[place][0]
            for more in found[place][1:]:
                total = total + more
            out_ref[place * block : place * block + block, lanes] = total.astype(BF16)


def key_gradient(query_rows, key_rows, value_rows, grad_rows, second_scale):
    return pl.pallas_call(
        key_gradient_body,
        out_shape=jax.ShapeDtypeStruct(query_rows.shape, BF16),
        in_specs=[pl.BlockSpec(memory_space=pltpu.SMEM)] + 4 * [pl.BlockSpec(memory_space=pltpu.VMEM)],
        out_specs=pl.BlockSpec(memory_space=pltpu.VMEM),
        compiler_params=pltpu.CompilerParams(vmem_limit_bytes=24 * MIB),
        name="key_gradient",
    )(second_scale, query_rows, key_rows, value_rows, grad_rows)


def first_message_body(factor_ref, weight_ref, out_ref, own_ref):
    shards = out_ref.shape[0]
    rows, rank = factor_ref.shape
    half = rank // 2
    share = (out_ref.shape[1] - rows) // 2
    core = lax.axis_index("tp")
    ranks = lax.broadcasted_iota(jnp.int32, (rank, half), 0)
    places = lax.broadcasted_iota(jnp.int32, (rank, half), 1)
    pair = sum((places >= i * shards).astype(jnp.int32) for i in range(1, half // shards))
    wanted = (places - pair * shards) * (rank // shards) + 2 * pair
    factor = factor_ref[...]
    mine = dot32(factor, (ranks == wanted + core).astype(F32).astype(BF16)).astype(BF16)
    other = dot32(factor, (ranks == wanted + 1 - core).astype(F32).astype(BF16)).astype(BF16)
    own_ref[:, :half] = mine
    own_ref[:, half:] = other
    start = pl.multiple_of(lax.axis_index("rep") * share, share)
    old = weight_ref[pl.ds(start, share), :].astype(BF16)
    out_ref[:, :rows, :] = jnp.broadcast_to(mine[None], (shards, rows, half))
    for i in range(2):
        piece = old[:, i * half : i * half + half]
        out_ref[:, rows + i * share : rows + i * share + share, :] = jnp.broadcast_to(
            piece[None], (shards, share, half)
        )


def first_message(factor, weight, shards, reps):
    rows, rank = factor.shape
    half = rank // 2
    return pl.pallas_call(
        first_message_body,
        out_shape=(
            jax.ShapeDtypeStruct((shards, rows + 2 * (rows // reps), half), BF16),
            jax.ShapeDtypeStruct((rows, rank), BF16),
        ),
        in_specs=2 * [VMEM_SPEC],
        out_specs=(VMEM_SPEC, VMEM_SPEC),
        compiler_params=pltpu.CompilerParams(vmem_limit_bytes=8 * MIB),
        name="first_message",
    )(factor, weight)


def projected_sums_body(tokens_ref, sent_ref, grad_ref, out_ref, laid_ref):
    shards, _, half = sent_ref.shape
    length, width = tokens_ref.shape
    rows = width // shards
    cols = grad_ref.shape[1]
    pairs = half // shards
    factor = sent_ref[:, :rows, :].reshape(width, half)
    reduced = dot32(tokens_ref[...], factor).T
    high = reduced.astype(BF16)
    low = (reduced - high.astype(F32)).astype(BF16)
    tiles = cols // 128
    for i in range(2):
        grads = grad_ref[i * length : i * length + length, :]
        sums = dot32(high, grads) + dot32(low, grads)
        for pair in range(pairs):
            for tile in range(tiles):
                place = (pair * 2 + i) * tiles + tile
                laid_ref[pl.ds(place, shards, 2 * pairs * tiles), :] = sums[
                    pair * shards : pair * shards + shards, tile * 128 : tile * 128 + 128
                ]
    out_ref[...] = laid_ref[...].astype(BF16)


def projected_sums(tokens, sent, grads):
    half = sent.shape[2]
    total = half * 2 * grads.shape[1] // 128
    return pl.pallas_call(
        projected_sums_body,
        out_shape=jax.ShapeDtypeStruct((total, 128), BF16),
        in_specs=3 * [VMEM_SPEC],
        out_specs=VMEM_SPEC,
        scratch_shapes=[pltpu.VMEM((total, 128), F32)],
        cost_estimate=pl.CostEstimate(
            flops=4 * tokens.size * half, bytes_accessed=2 * tokens.size, transcendentals=0
        ),
        compiler_params=pltpu.CompilerParams(vmem_limit_bytes=16 * MIB),
        name="projected_sums",
    )(tokens, sent, grads)


def summed_body(arrived_ref, out_ref):
    total = jnp.sum(arrived_ref[...].astype(F32), axis=0)
    out_ref[...] = jnp.broadcast_to(total[None], out_ref.shape)


def summed(arrived, count):
    return pl.pallas_call(
        summed_body,
        out_shape=jax.ShapeDtypeStruct((count, *arrived.shape[1:]), F32),
        in_specs=[VMEM_SPEC],
        out_specs=VMEM_SPEC,
        compiler_params=pltpu.CompilerParams(vmem_limit_bytes=4 * MIB),
        name="summed",
    )(arrived)


def moments_step_body(part_ref, moments_ref, message_ref, first_ref, second_ref):
    shards = message_ref.shape[0]
    lines = first_ref.shape[0]
    core = lax.axis_index("tp")
    total = part_ref[:lines, :]
    for i in range(lines, part_ref.shape[0], lines):
        total = total + part_ref[i : i + lines, :]
    new_first = 0.9 * moments_ref[:lines, :] + 0.1 * total
    new_second = 0.95 * moments_ref[lines:, :] + 0.05 * total * total
    first_ref[...] = new_first
    second_ref[...] = new_second
    direction = (new_first / (jnp.sqrt(new_second) + 1e-08)).astype(BF16).astype(F32)
    squares = direction * direction
    squares = jnp.sum(jnp.sum(squares, axis=1, keepdims=True), axis=0, keepdims=True)
    quarter = lines // 8
    own = []
    for i in range(4):
        base = i * 2 * quarter
        own.append(
            jnp.where(
                core == 0,
                direction[base : base + quarter],
                direction[base + quarter : base + 2 * quarter],
            )
        )
    high = squares.astype(BF16).astype(F32)
    middle = (squares - high).astype(BF16).astype(F32)
    low = squares - high - middle
    lane = lax.broadcasted_iota(jnp.int32, (lines // 2, 128), 1)
    row = lax.broadcasted_iota(jnp.int32, (lines // 2, 128), 0)
    packed = jnp.where(lane == 0, high, jnp.where(lane == 1, middle, jnp.where(lane == 2, low, 0.0)))
    own.append(jnp.where(row == 0, packed, 0.0))
    message = jnp.concatenate(own, axis=0).astype(BF16)
    message_ref[...] = jnp.broadcast_to(message[None], (shards, lines, 128))


def moments_step(part, moments, shards):
    lines = moments.shape[0] // 2
    return pl.pallas_call(
        moments_step_body,
        out_shape=(
            jax.ShapeDtypeStruct((shards, lines, 128), BF16),
            jax.ShapeDtypeStruct((lines, 128), F32),
            jax.ShapeDtypeStruct((lines, 128), F32),
        ),
        in_specs=2 * [VMEM_SPEC],
        out_specs=3 * (VMEM_SPEC,),
        compiler_params=pltpu.CompilerParams(vmem_limit_bytes=4 * MIB),
        name="moments_step",
    )(part, moments)


def new_weights_body(
    gathered_ref, sent_ref, swapped_ref, old_ref, own_ref, weight_ref,
    copies_ref, update_ref, weight_out_ref, laid_ref,
):
    shards = sent_ref.shape[0]
    lines = gathered_ref.shape[0] // shards
    width, half = swapped_ref.shape
    rows = width // shards
    reps, share = copies_ref.shape[1:3]
    cols = weight_ref.shape[1]
    tiles = cols // 128
    pairs = half // shards
    core = lax.axis_index("tp")
    laid_ref[...] = gathered_ref[...].astype(F32)

    def line(place):
        return laid_ref[pl.ds(place, shards, lines), :]

    def directions(parity):
        return jnp.concatenate(
            [
                jnp.concatenate(
                    [line((parity * pairs + pair) * tiles + tile) for tile in range(tiles)], axis=1
                )
                for pair in range(pairs)
            ],
            axis=0,
        )

    even, odd = directions(0), directions(1)
    mine = jnp.where(core == 0, even, odd).astype(BF16)
    other = jnp.where(core == 0, odd, even).astype(BF16)
    squares = line(lines // 2)
    squares = jnp.sum(jnp.sum(squares, axis=1, keepdims=True), axis=0, keepdims=True)
    rate = lax.rsqrt(squares / (RANK * KW) + 1e-06)
    update = (dot32(own_ref[:, :half], mine) + dot32(own_ref[:, half:], other)) * rate
    update_ref[...] = update
    weight_out_ref[...] = weight_ref[...] - 0.1 * update
    pieces = 4
    group = shards // pieces
    for piece in range(pieces):
        owners = slice(piece * group, piece * group + group)
        factor = sent_ref[owners, :rows, :].reshape(group * rows, half)
        swapped = swapped_ref[piece * group * rows : (piece + 1) * group * rows, :]
        step = (dot32(factor, mine) + dot32(swapped, other)) * (0.1 * rate)
        for i in range(cols // half):
            lanes = slice(i * half, i * half + half)
            old = old_ref[owners, :, i * share : i * share + share, :].astype(F32)
            copies_ref[owners, :, :, lanes] = (
                old - step[:, lanes].reshape(group, reps, share, half)
            ).astype(BF16)


def new_weights(gathered, sent, swapped, old, own_factor, weight):
    shards, reps = old.shape[:2]
    rows, cols = weight.shape
    return pl.pallas_call(
        new_weights_body,
        out_shape=(
            jax.ShapeDtypeStruct((shards, reps, rows // reps, cols), BF16),
            jax.ShapeDtypeStruct((rows, cols), F32),
            jax.ShapeDtypeStruct((rows, cols), F32),
        ),
        in_specs=6 * [VMEM_SPEC],
        out_specs=3 * (VMEM_SPEC,),
        scratch_shapes=[pltpu.VMEM(gathered.shape, F32)],
        cost_estimate=pl.CostEstimate(
            flops=4 * swapped.size * cols, bytes_accessed=8 * swapped.size, transcendentals=0
        ),
        compiler_params=pltpu.CompilerParams(vmem_limit_bytes=20 * MIB),
        name="new_weights",
    )(gathered, sent, swapped, old, own_factor, weight)


def on_device(
    tokens_in,
    query_two,
    key_two,
    values,
    out_grad,
    second_scale,
    factor,
    weight,
    first_moment,
    second_moment,
):
    shards = lax.axis_size("fs")
    reps = lax.axis_size("rep")
    rep = lax.axis_index("rep")
    core = lax.axis_index("tp")
    half = factor.shape[1] // 2
    rows, cols = weight.shape
    tiles = cols // 128
    own_rows = first_moment.shape[0]
    pairs = own_rows // 2
    lines = own_rows * 2 * tiles

    message, own_factor = first_message(factor, weight, shards, reps)
    sent = lax.all_to_all(message, "fs", 0, 0, tiled=True)
    old_mine = sent[:, rows:]
    factor_mine = sent[:, :rows].reshape(-1, half)

    moments = lax.all_gather(jnp.concatenate([first_moment, second_moment], 0), "tp")
    moments = moments.reshape(2, 2, pairs, 2, tiles, 128)
    moments = moments.transpose(1, 3, 2, 0, 4, 5).reshape(2 * lines, 128)

    key_grad = key_gradient(query_two, key_two, values, out_grad, second_scale)
    key_both = lax.all_gather(key_grad, "tp", tiled=True)
    moments, key_both = lax.optimization_barrier((moments, key_both))

    sums = projected_sums(tokens_in, sent, key_both)
    arrived = lax.all_to_all(sums.reshape(shards, lines // 2, 128), "fs", 0, 0, tiled=True)
    part = lax.all_to_all(summed(arrived, 2 * reps), ("rep", "tp"), 0, 0, tiled=True)
    message, new_first, new_second = moments_step(
        part.reshape(reps * lines, 128), moments, shards
    )
    gathered = lax.all_to_all(message, "fs", 0, 0, tiled=True)

    old_all = jnp.zeros((shards, reps, *old_mine.shape[1:]), BF16)
    old_all = lax.dynamic_update_index_in_dim(old_all, old_mine, rep, 1)
    for i in (2, 1, 3):
        came = lax.ppermute(old_mine, "rep", [(j, (j + i) % reps) for j in range(reps)])
        old_all = lax.dynamic_update_index_in_dim(old_all, came, (rep + reps - i) % reps, 1)
    factor_other = lax.ppermute(factor_mine, "tp", [(0, 1), (1, 0)])

    copies, update_step, new_weight = new_weights(
        gathered.reshape(shards * lines, 128), sent, factor_other, old_all, own_factor, weight
    )

    def own_entries(value):
        value = value.reshape(2, pairs, 2, tiles * 128)
        value = jnp.where(core == 0, value[:, :, 0], value[:, :, 1])
        return jnp.stack([value[0], value[1]], axis=1).reshape(own_rows, cols)

    return (
        new_weight,
        copies.reshape(-1, cols),
        update_step,
        own_entries(new_first),
        own_entries(new_second),
    )


def solution(mesh):
    in_specs = (
        P(("fs", "rep"), None),
        P(("fs", "rep"), "tp"),
        P(("fs", "rep"), "tp"),
        P(("fs", "rep"), "tp"),
        P(("fs", "rep"), "tp"),
        P("tp"),
        P("fs", None),
        P("fs", "tp"),
        P("fs", "tp"),
        P("fs", "tp"),
    )
    out_specs = (P("fs", "tp"), P(None, "tp"), P("fs", "tp"), P("fs", "tp"), P("fs", "tp"))

    return jax.shard_map(
        on_device, mesh=mesh, in_specs=in_specs, out_specs=out_specs, check_vma=False
    )
```

```python
import jax
import jax.numpy as jnp
from jax import lax
from jax.experimental import pallas as pl
from jax.experimental.pallas import tpu as pltpu
from jax.sharding import PartitionSpec as P


RANK = 256
KW = 512
BF16 = jnp.bfloat16
F32 = jnp.float32

MIB = 1024 * 1024
VMEM_SPEC = pl.BlockSpec(memory_space=pltpu.VMEM)


def dot32(left, right):
    return jnp.dot(left, right, preferred_element_type=F32)


def dot_rows(left, right):
    return lax.dot_general(left, right, (((1,), (1,)), ((), ())), preferred_element_type=F32)


def key_gradient_body(scale_ref, query_ref, key_ref, value_ref, grad_ref, out_ref):
    length = query_ref.shape[0]
    block = length // 2
    heads = scale_ref.shape[0]
    dim = query_ref.shape[1] // heads
    wide = value_ref.shape[1] // heads
    inv_root = dim ** (-0.5)
    pair = 2 * dim
    lane = lax.broadcasted_iota(jnp.int32, (block, pair), 1)
    later = lax.broadcasted_iota(jnp.int32, (block, block), 0) > lax.broadcasted_iota(
        jnp.int32, (block, block), 1
    )
    for first in range(0, heads, 2):
        lanes = slice(first * dim, first * dim + pair)
        found = [[], []]
        for side in range(2):
            head = first + side
            span = slice(head * wide, head * wide + wide)
            for step in range(2):
                rows = slice(step * block, step * block + block)
                seen = block * (step + 1)
                own = query_ref[rows, lanes].astype(F32) * inv_root
                own = jnp.where((lane >= dim) == (side == 1), own, 0.0).astype(BF16)
                scores = dot_rows(key_ref[:seen, lanes], own)
                last = jnp.where(later, -1e30, scores[seen - block :])
                scores = jnp.concatenate([scores[: seen - block], last], axis=0) if step else last
                exps = jnp.exp(scores - jnp.max(scores, axis=0, keepdims=True))
                total = jnp.sum(exps, axis=0, keepdims=True)
                attn_grad = dot_rows(value_ref[:seen, span], grad_ref[rows, span])
                weights_map = exps / total
                inner = jnp.sum(weights_map * attn_grad, axis=0, keepdims=True)
                score_grad = (-scale_ref[head] * weights_map * (attn_grad - inner)).astype(BF16)
                for place in range(step + 1):
                    found[place].append(
                        dot32(score_grad[place * block : place * block + block], own)
                    )
        for place in range(2):
            total = found[place][0]
            for more in found[place][1:]:
                total = total + more
            out_ref[place * block : place * block + block, lanes] = total.astype(BF16)


def key_gradient(query_rows, key_rows, value_rows, grad_rows, second_scale):
    return pl.pallas_call(
        key_gradient_body,
        out_shape=jax.ShapeDtypeStruct(query_rows.shape, BF16),
        in_specs=[pl.BlockSpec(memory_space=pltpu.SMEM)] + 4 * [pl.BlockSpec(memory_space=pltpu.VMEM)],
        out_specs=pl.BlockSpec(memory_space=pltpu.VMEM),
        compiler_params=pltpu.CompilerParams(vmem_limit_bytes=24 * MIB),
        name="key_gradient",
    )(second_scale, query_rows, key_rows, value_rows, grad_rows)


def first_message_body(
    factor_hbm, weight_hbm, out_hbm, own_ref, factor_ref, weight_ref, out_ref, sems
):
    shards = out_ref.shape[0]
    rows, rank = factor_ref.shape
    half = rank // 2
    share = weight_ref.shape[0]
    start = pl.multiple_of(lax.axis_index("rep") * share, share)
    factor_copy = pltpu.make_async_copy(factor_hbm, factor_ref, sems.at[0])
    weight_copy = pltpu.make_async_copy(weight_hbm.at[pl.ds(start, share), :], weight_ref, sems.at[1])
    factor_copy.start()
    weight_copy.start()
    core = lax.axis_index("tp")
    ranks = lax.broadcasted_iota(jnp.int32, (rank, half), 0)
    places = lax.broadcasted_iota(jnp.int32, (rank, half), 1)
    pair = sum((places >= i * shards).astype(jnp.int32) for i in range(1, half // shards))
    wanted = (places - pair * shards) * (rank // shards) + 2 * pair
    pick = (ranks == wanted + core).astype(F32).astype(BF16)
    pick_other = (ranks == wanted + 1 - core).astype(F32).astype(BF16)
    factor_copy.wait()
    factor = factor_ref[...]
    mine = dot32(factor, pick).astype(BF16)
    own_ref[:, :half] = mine
    own_ref[:, half:] = dot32(factor, pick_other).astype(BF16)
    out_ref[:, :rows, :] = jnp.broadcast_to(mine[None], (shards, rows, half))
    weight_copy.wait()
    old = weight_ref[...].astype(BF16)
    for i in range(2):
        piece = old[:, i * half : i * half + half]
        out_ref[:, rows + i * share : rows + i * share + share, :] = jnp.broadcast_to(
            piece[None], (shards, share, half)
        )
    out_copy = pltpu.make_async_copy(out_ref, out_hbm, sems.at[0])
    out_copy.start()
    out_copy.wait()


def first_message(factor, weight, shards, reps):
    rows, rank = factor.shape
    half = rank // 2
    share = rows // reps
    message = (shards, rows + 2 * share, half)
    any_spec = pl.BlockSpec(memory_space=pltpu.HBM)
    return pl.pallas_call(
        first_message_body,
        out_shape=(
            jax.ShapeDtypeStruct(message, BF16),
            jax.ShapeDtypeStruct((rows, rank), BF16),
        ),
        in_specs=2 * [any_spec],
        out_specs=(any_spec, VMEM_SPEC),
        scratch_shapes=[
            pltpu.VMEM((rows, rank), BF16),
            pltpu.VMEM((share, weight.shape[1]), F32),
            pltpu.VMEM(message, BF16),
            pltpu.SemaphoreType.DMA((2,)),
        ],
        compiler_params=pltpu.CompilerParams(vmem_limit_bytes=60 * MIB),
        name="first_message",
    )(factor, weight)


def projected_sums_body(tokens_ref, sent_ref, grad_ref, out_ref, laid_ref):
    shards, _, half = sent_ref.shape
    length, width = tokens_ref.shape
    rows = width // shards
    cols = grad_ref.shape[1]
    pairs = half // shards
    factor = sent_ref[:, :rows, :].reshape(width, half)
    reduced = dot32(tokens_ref[...], factor).T
    high = reduced.astype(BF16)
    low = (reduced - high.astype(F32)).astype(BF16)
    tiles = cols // 128
    for i in range(2):
        grads = grad_ref[i * length : i * length + length, :]
        sums = dot32(high, grads) + dot32(low, grads)
        for pair in range(pairs):
            for tile in range(tiles):
                place = (pair * 2 + i) * tiles + tile
                laid_ref[pl.ds(place, shards, 2 * pairs * tiles), :] = sums[
                    pair * shards : pair * shards + shards, tile * 128 : tile * 128 + 128
                ]
    out_ref[...] = laid_ref[...].astype(BF16)


def projected_sums(tokens, sent, grads):
    half = sent.shape[2]
    total = half * 2 * grads.shape[1] // 128
    return pl.pallas_call(
        projected_sums_body,
        out_shape=jax.ShapeDtypeStruct((total, 128), BF16),
        in_specs=3 * [VMEM_SPEC],
        out_specs=VMEM_SPEC,
        scratch_shapes=[pltpu.VMEM((total, 128), F32)],
        cost_estimate=pl.CostEstimate(
            flops=4 * tokens.size * half, bytes_accessed=2 * tokens.size, transcendentals=0
        ),
        compiler_params=pltpu.CompilerParams(vmem_limit_bytes=16 * MIB),
        name="projected_sums",
    )(tokens, sent, grads)


def summed_body(arrived_ref, out_ref):
    total = jnp.sum(arrived_ref[...].astype(F32), axis=0)
    out_ref[...] = jnp.broadcast_to(total[None], out_ref.shape)


def summed(arrived, count):
    return pl.pallas_call(
        summed_body,
        out_shape=jax.ShapeDtypeStruct((count, *arrived.shape[1:]), F32),
        in_specs=[VMEM_SPEC],
        out_specs=VMEM_SPEC,
        compiler_params=pltpu.CompilerParams(vmem_limit_bytes=4 * MIB),
        name="summed",
    )(arrived)


def moments_step_body(part_ref, moments_ref, message_ref, first_ref, second_ref):
    lines = first_ref.shape[0]
    core = lax.axis_index("tp")
    total = part_ref[:lines, :]
    for i in range(lines, part_ref.shape[0], lines):
        total = total + part_ref[i : i + lines, :]
    new_first = 0.9 * moments_ref[:lines, :] + 0.1 * total
    new_second = 0.95 * moments_ref[lines:, :] + 0.05 * total * total
    first_ref[...] = new_first
    second_ref[...] = new_second
    direction = (new_first / (jnp.sqrt(new_second) + 1e-08)).astype(BF16).astype(F32)
    squares = direction * direction
    squares = jnp.sum(jnp.sum(squares, axis=1, keepdims=True), axis=0, keepdims=True)
    own = []
    tiles = lines // 8
    for pair in range(2):
        made = []
        for parity in range(2):
            base = (parity * 2 + pair) * 2 * tiles
            for tile in range(tiles):
                made.append(
                    jnp.where(
                        core == 0,
                        direction[base + tile : base + tile + 1],
                        direction[base + tiles + tile : base + tiles + tile + 1],
                    )
                )
        own.append(jnp.concatenate(made, axis=1))
    high = squares.astype(BF16).astype(F32)
    middle = (squares - high).astype(BF16).astype(F32)
    low = squares - high - middle
    lane = lax.broadcasted_iota(jnp.int32, (1, 128), 1)
    packed = jnp.where(lane == 0, high, jnp.where(lane == 1, middle, jnp.where(lane == 2, low, 0.0)))
    own[0] = jnp.concatenate([own[0], packed], axis=1)
    own[1] = jnp.concatenate([own[1], jnp.zeros_like(packed)], axis=1)
    message = jnp.concatenate(own, axis=0).astype(BF16)
    message_ref[...] = jnp.broadcast_to(message[None], message_ref.shape)


def moments_step(part, moments, shards):
    lines = moments.shape[0] // 2
    return pl.pallas_call(
        moments_step_body,
        out_shape=(
            jax.ShapeDtypeStruct((shards, 2, lines * 32 + 128), BF16),
            jax.ShapeDtypeStruct((lines, 128), F32),
            jax.ShapeDtypeStruct((lines, 128), F32),
        ),
        in_specs=2 * [VMEM_SPEC],
        out_specs=3 * (VMEM_SPEC,),
        compiler_params=pltpu.CompilerParams(vmem_limit_bytes=4 * MIB),
        name="moments_step",
    )(part, moments)


def new_weights_body(
    gathered_ref, sent_ref, swapped_ref, old_ref, own_ref, weight_ref,
    copies_ref, update_ref, weight_out_ref,
):
    shards = sent_ref.shape[0]
    width, half = swapped_ref.shape
    rows = width // shards
    reps, share = copies_ref.shape[1:3]
    cols = weight_ref.shape[1]
    tiles = cols // 128
    pairs = half // shards
    core = lax.axis_index("tp")

    def line(pair, place):
        return gathered_ref[:, pair, place * 128 : place * 128 + 128].astype(F32)

    def directions(parity):
        return jnp.concatenate(
            [
                jnp.concatenate(
                    [line(pair, parity * tiles + tile) for tile in range(tiles)], axis=1
                )
                for pair in range(pairs)
            ],
            axis=0,
        )

    even, odd = directions(0), directions(1)
    mine = jnp.where(core == 0, even, odd).astype(BF16)
    other = jnp.where(core == 0, odd, even).astype(BF16)
    squares = line(0, 2 * tiles)
    squares = jnp.sum(jnp.sum(squares, axis=1, keepdims=True), axis=0, keepdims=True)
    rate = lax.rsqrt(squares / (RANK * KW) + 1e-06)
    both = jnp.concatenate([mine, other], axis=0)
    pieces = 4
    group = shards // pieces
    for piece in range(pieces):
        owners = slice(piece * group, piece * group + group)
        factor = jnp.concatenate(
            [
                sent_ref[owners, :rows, :].reshape(group * rows, half),
                swapped_ref[piece * group * rows : (piece + 1) * group * rows, :],
            ],
            axis=1,
        )
        step = dot32(factor, both) * (0.1 * rate)
        for i in range(cols // half):
            lanes = slice(i * half, i * half + half)
            old = old_ref[owners, :, i * share : i * share + share, :].astype(F32)
            copies_ref[owners, :, :, lanes] = (
                old - step[:, lanes].reshape(group, reps, share, half)
            ).astype(BF16)
    update = dot32(own_ref[...], both) * rate
    update_ref[...] = update
    weight_out_ref[...] = weight_ref[...] - 0.1 * update


def new_weights(gathered, sent, swapped, old, own_factor, weight):
    shards, reps = old.shape[:2]
    rows, cols = weight.shape
    return pl.pallas_call(
        new_weights_body,
        out_shape=(
            jax.ShapeDtypeStruct((shards, reps, rows // reps, cols), BF16),
            jax.ShapeDtypeStruct((rows, cols), F32),
            jax.ShapeDtypeStruct((rows, cols), F32),
        ),
        in_specs=6 * [VMEM_SPEC],
        out_specs=3 * (VMEM_SPEC,),
        cost_estimate=pl.CostEstimate(
            flops=4 * swapped.size * cols, bytes_accessed=8 * swapped.size, transcendentals=0
        ),
        compiler_params=pltpu.CompilerParams(vmem_limit_bytes=20 * MIB),
        name="new_weights",
    )(gathered, sent, swapped, old, own_factor, weight)


def on_device(
    tokens_in,
    query_two,
    key_two,
    values,
    out_grad,
    second_scale,
    factor,
    weight,
    first_moment,
    second_moment,
):
    shards = lax.axis_size("fs")
    reps = lax.axis_size("rep")
    rep = lax.axis_index("rep")
    core = lax.axis_index("tp")
    half = factor.shape[1] // 2
    rows, cols = weight.shape
    tiles = cols // 128
    own_rows = first_moment.shape[0]
    pairs = own_rows // 2
    lines = own_rows * 2 * tiles

    message, own_factor = first_message(factor, weight, shards, reps)
    sent = lax.all_to_all(message, "fs", 0, 0, tiled=True)
    old_mine = sent[:, rows:]
    factor_mine = sent[:, :rows].reshape(-1, half)

    moments = lax.all_gather(jnp.concatenate([first_moment, second_moment], 0), "tp")
    moments = moments.reshape(2, 2, pairs, 2, tiles, 128)
    moments = moments.transpose(1, 3, 2, 0, 4, 5).reshape(2 * lines, 128)

    key_grad = key_gradient(query_two, key_two, values, out_grad, second_scale)
    key_both = lax.all_gather(key_grad, "tp", tiled=True)
    moments, key_both = lax.optimization_barrier((moments, key_both))

    sums = projected_sums(tokens_in, sent, key_both)
    arrived = lax.all_to_all(sums.reshape(shards, lines // 2, 128), "fs", 0, 0, tiled=True)
    part = lax.all_to_all(summed(arrived, 2 * reps), ("rep", "tp"), 0, 0, tiled=True)
    message, new_first, new_second = moments_step(
        part.reshape(reps * lines, 128), moments, shards
    )
    gathered = lax.all_to_all(message, "fs", 0, 0, tiled=True)

    old_all = jnp.zeros((shards, reps, *old_mine.shape[1:]), BF16)
    old_all = lax.dynamic_update_index_in_dim(old_all, old_mine, rep, 1)
    for i in (2, 1, 3):
        came = lax.ppermute(old_mine, "rep", [(j, (j + i) % reps) for j in range(reps)])
        old_all = lax.dynamic_update_index_in_dim(old_all, came, (rep + reps - i) % reps, 1)
    factor_other = lax.ppermute(factor_mine, "tp", [(0, 1), (1, 0)])

    copies, update_step, new_weight = new_weights(
        gathered, sent, factor_other, old_all, own_factor, weight
    )

    def own_entries(value):
        value = value.reshape(2, pairs, 2, tiles * 128)
        value = jnp.where(core == 0, value[:, :, 0], value[:, :, 1])
        return jnp.stack([value[0], value[1]], axis=1).reshape(own_rows, cols)

    return (
        new_weight,
        copies.reshape(-1, cols),
        update_step,
        own_entries(new_first),
        own_entries(new_second),
    )


def solution(mesh):
    in_specs = (
        P(("fs", "rep"), None),
        P(("fs", "rep"), "tp"),
        P(("fs", "rep"), "tp"),
        P(("fs", "rep"), "tp"),
        P(("fs", "rep"), "tp"),
        P("tp"),
        P("fs", None),
        P("fs", "tp"),
        P("fs", "tp"),
        P("fs", "tp"),
    )
    out_specs = (P("fs", "tp"), P(None, "tp"), P("fs", "tp"), P("fs", "tp"), P("fs", "tp"))

    return jax.shard_map(
        on_device, mesh=mesh, in_specs=in_specs, out_specs=out_specs, check_vma=False
    )
```

```python
import jax
import jax.numpy as jnp
from jax import lax
from jax.experimental import pallas as pl
from jax.experimental.pallas import tpu as pltpu
from jax.sharding import PartitionSpec as P


RANK = 256
KW = 512
BF16 = jnp.bfloat16
F32 = jnp.float32

MIB = 1024 * 1024
VMEM_SPEC = pl.BlockSpec(memory_space=pltpu.VMEM)


def dot32(left, right):
    return jnp.dot(left, right, preferred_element_type=F32)


def dot_rows(left, right):
    return lax.dot_general(left, right, (((1,), (1,)), ((), ())), preferred_element_type=F32)


def key_gradient_body(scale_ref, query_ref, key_ref, value_ref, grad_ref, out_ref):
    length = query_ref.shape[0]
    block = length // 2
    heads = scale_ref.shape[0]
    dim = query_ref.shape[1] // heads
    wide = value_ref.shape[1] // heads
    inv_root = dim ** (-0.5)
    pair = 2 * dim
    lane = lax.broadcasted_iota(jnp.int32, (block, pair), 1)
    later = lax.broadcasted_iota(jnp.int32, (block, block), 0) > lax.broadcasted_iota(
        jnp.int32, (block, block), 1
    )
    for first in range(0, heads, 2):
        lanes = slice(first * dim, first * dim + pair)
        found = [[], []]
        for side in range(2):
            head = first + side
            span = slice(head * wide, head * wide + wide)
            for step in range(2):
                rows = slice(step * block, step * block + block)
                seen = block * (step + 1)
                own = query_ref[rows, lanes].astype(F32) * inv_root
                own = jnp.where((lane >= dim) == (side == 1), own, 0.0).astype(BF16)
                scores = dot_rows(key_ref[:seen, lanes], own)
                last = jnp.where(later, -1e30, scores[seen - block :])
                scores = jnp.concatenate([scores[: seen - block], last], axis=0) if step else last
                exps = jnp.exp(scores - jnp.max(scores, axis=0, keepdims=True))
                total = jnp.sum(exps, axis=0, keepdims=True)
                attn_grad = dot_rows(value_ref[:seen, span], grad_ref[rows, span])
                weights_map = exps / total
                inner = jnp.sum(weights_map * attn_grad, axis=0, keepdims=True)
                score_grad = (-scale_ref[head] * weights_map * (attn_grad - inner)).astype(BF16)
                for place in range(step + 1):
                    found[place].append(
                        dot32(score_grad[place * block : place * block + block], own)
                    )
        for place in range(2):
            total = found[place][0]
            for more in found[place][1:]:
                total = total + more
            out_ref[place * block : place * block + block, lanes] = total.astype(BF16)


def key_gradient(query_rows, key_rows, value_rows, grad_rows, second_scale):
    return pl.pallas_call(
        key_gradient_body,
        out_shape=jax.ShapeDtypeStruct(query_rows.shape, BF16),
        in_specs=[pl.BlockSpec(memory_space=pltpu.SMEM)] + 4 * [pl.BlockSpec(memory_space=pltpu.VMEM)],
        out_specs=pl.BlockSpec(memory_space=pltpu.VMEM),
        compiler_params=pltpu.CompilerParams(vmem_limit_bytes=24 * MIB),
        name="key_gradient",
    )(second_scale, query_rows, key_rows, value_rows, grad_rows)


def first_message_body(
    factor_hbm, weight_hbm, out_hbm, own_ref, factor_ref, weight_ref, out_ref, sems
):
    shards = out_ref.shape[0]
    rows, rank = factor_ref.shape
    half = rank // 2
    share = weight_ref.shape[0]
    start = pl.multiple_of(lax.axis_index("rep") * share, share)
    factor_copy = pltpu.make_async_copy(factor_hbm, factor_ref, sems.at[0])
    weight_copy = pltpu.make_async_copy(weight_hbm.at[pl.ds(start, share), :], weight_ref, sems.at[1])
    factor_copy.start()
    weight_copy.start()
    core = lax.axis_index("tp")
    ranks = lax.broadcasted_iota(jnp.int32, (rank, half), 0)
    places = lax.broadcasted_iota(jnp.int32, (rank, half), 1)
    pair = sum((places >= i * shards).astype(jnp.int32) for i in range(1, half // shards))
    wanted = (places - pair * shards) * (rank // shards) + 2 * pair
    pick = (ranks == wanted + core).astype(F32).astype(BF16)
    pick_other = (ranks == wanted + 1 - core).astype(F32).astype(BF16)
    factor_copy.wait()
    factor = factor_ref[...]
    mine = dot32(factor, pick).astype(BF16)
    own_ref[:, :half] = mine
    out_ref[:, :rows, :] = jnp.broadcast_to(mine[None], (shards, rows, half))
    weight_copy.wait()
    old = weight_ref[...].astype(BF16)
    for i in range(2):
        piece = old[:, i * half : i * half + half]
        out_ref[:, rows + i * share : rows + i * share + share, :] = jnp.broadcast_to(
            piece[None], (shards, share, half)
        )
    out_copy = pltpu.make_async_copy(out_ref, out_hbm, sems.at[0])
    out_copy.start()
    own_ref[:, half:] = dot32(factor, pick_other).astype(BF16)
    out_copy.wait()


def first_message(factor, weight, shards, reps):
    rows, rank = factor.shape
    half = rank // 2
    share = rows // reps
    message = (shards, rows + 2 * share, half)
    any_spec = pl.BlockSpec(memory_space=pltpu.HBM)
    return pl.pallas_call(
        first_message_body,
        out_shape=(
            jax.ShapeDtypeStruct(message, BF16),
            jax.ShapeDtypeStruct((rows, rank), BF16),
        ),
        in_specs=2 * [any_spec],
        out_specs=(any_spec, VMEM_SPEC),
        scratch_shapes=[
            pltpu.VMEM((rows, rank), BF16),
            pltpu.VMEM((share, weight.shape[1]), F32),
            pltpu.VMEM(message, BF16),
            pltpu.SemaphoreType.DMA((2,)),
        ],
        compiler_params=pltpu.CompilerParams(vmem_limit_bytes=60 * MIB),
        name="first_message",
    )(factor, weight)


def projected_sums_body(tokens_ref, sent_ref, grad_ref, out_ref, laid_ref):
    shards, _, half = sent_ref.shape
    length, width = tokens_ref.shape
    rows = width // shards
    cols = grad_ref.shape[1]
    pairs = half // shards
    factor = sent_ref[:, :rows, :].reshape(width, half)
    reduced = dot32(tokens_ref[...], factor).T
    high = reduced.astype(BF16)
    low = (reduced - high.astype(F32)).astype(BF16)
    tiles = cols // 128
    for i in range(2):
        grads = grad_ref[i * length : i * length + length, :]
        sums = dot32(high, grads) + dot32(low, grads)
        for pair in range(pairs):
            for tile in range(tiles):
                place = (pair * 2 + i) * tiles + tile
                laid_ref[pl.ds(place, shards, 2 * pairs * tiles), :] = sums[
                    pair * shards : pair * shards + shards, tile * 128 : tile * 128 + 128
                ]
    out_ref[...] = laid_ref[...].astype(BF16)


def projected_sums(tokens, sent, grads):
    half = sent.shape[2]
    total = half * 2 * grads.shape[1] // 128
    return pl.pallas_call(
        projected_sums_body,
        out_shape=jax.ShapeDtypeStruct((total, 128), BF16),
        in_specs=3 * [VMEM_SPEC],
        out_specs=VMEM_SPEC,
        scratch_shapes=[pltpu.VMEM((total, 128), F32)],
        cost_estimate=pl.CostEstimate(
            flops=4 * tokens.size * half, bytes_accessed=2 * tokens.size, transcendentals=0
        ),
        compiler_params=pltpu.CompilerParams(vmem_limit_bytes=16 * MIB),
        name="projected_sums",
    )(tokens, sent, grads)


def summed_body(arrived_ref, out_ref):
    total = jnp.sum(arrived_ref[...].astype(F32), axis=0)
    out_ref[...] = jnp.broadcast_to(total[None], out_ref.shape)


def summed(arrived, count):
    return pl.pallas_call(
        summed_body,
        out_shape=jax.ShapeDtypeStruct((count, *arrived.shape[1:]), F32),
        in_specs=[VMEM_SPEC],
        out_specs=VMEM_SPEC,
        compiler_params=pltpu.CompilerParams(vmem_limit_bytes=4 * MIB),
        name="summed",
    )(arrived)


def moments_step_body(part_ref, moments_ref, message_ref, first_ref, second_ref):
    lines = moments_ref.shape[0] // 2
    core = lax.axis_index("tp")
    total = part_ref[:lines, :]
    for i in range(lines, part_ref.shape[0], lines):
        total = total + part_ref[i : i + lines, :]
    new_first = 0.9 * moments_ref[:lines, :] + 0.1 * total
    new_second = 0.95 * moments_ref[lines:, :] + 0.05 * total * total
    direction = (new_first / (jnp.sqrt(new_second) + 1e-08)).astype(BF16).astype(F32)
    squares = direction * direction
    squares = jnp.sum(jnp.sum(squares, axis=1, keepdims=True), axis=0, keepdims=True)
    tiles = lines // 8

    def own_row(value, pair, parity):
        base = (parity * 2 + pair) * 2 * tiles
        return jnp.concatenate(
            [
                jnp.where(
                    core == 0,
                    value[base + tile : base + tile + 1],
                    value[base + tiles + tile : base + tiles + tile + 1],
                )
                for tile in range(tiles)
            ],
            axis=1,
        )

    for pair in range(2):
        for parity in range(2):
            row = pair * 2 + parity
            first_ref[row : row + 1, :] = own_row(new_first, pair, parity)
            second_ref[row : row + 1, :] = own_row(new_second, pair, parity)
    own = [
        jnp.concatenate([own_row(direction, pair, parity) for parity in range(2)], axis=1)
        for pair in range(2)
    ]
    high = squares.astype(BF16).astype(F32)
    middle = (squares - high).astype(BF16).astype(F32)
    low = squares - high - middle
    lane = lax.broadcasted_iota(jnp.int32, (1, 128), 1)
    packed = jnp.where(lane == 0, high, jnp.where(lane == 1, middle, jnp.where(lane == 2, low, 0.0)))
    own[0] = jnp.concatenate([own[0], packed], axis=1)
    own[1] = jnp.concatenate([own[1], jnp.zeros_like(packed)], axis=1)
    message = jnp.concatenate(own, axis=0).astype(BF16)
    message_ref[...] = jnp.broadcast_to(message[None], message_ref.shape)


def moments_step(part, moments, shards):
    lines = moments.shape[0] // 2
    return pl.pallas_call(
        moments_step_body,
        out_shape=(
            jax.ShapeDtypeStruct((shards, 2, lines * 32 + 128), BF16),
            jax.ShapeDtypeStruct((4, lines * 16), F32),
            jax.ShapeDtypeStruct((4, lines * 16), F32),
        ),
        in_specs=2 * [VMEM_SPEC],
        out_specs=3 * (VMEM_SPEC,),
        compiler_params=pltpu.CompilerParams(vmem_limit_bytes=4 * MIB),
        name="moments_step",
    )(part, moments)


def new_weights_body(
    gathered_ref, sent_ref, swapped_ref, old_ref, own_ref, weight_ref,
    copies_ref, update_ref, weight_out_ref,
):
    shards = sent_ref.shape[0]
    width, half = swapped_ref.shape
    rows = width // shards
    reps, share = copies_ref.shape[1:3]
    cols = weight_ref.shape[1]
    tiles = cols // 128
    pairs = half // shards
    core = lax.axis_index("tp")

    def line(pair, place):
        return gathered_ref[:, pair, place * 128 : place * 128 + 128].astype(F32)

    def directions(parity):
        return jnp.concatenate(
            [
                jnp.concatenate(
                    [line(pair, parity * tiles + tile) for tile in range(tiles)], axis=1
                )
                for pair in range(pairs)
            ],
            axis=0,
        )

    even, odd = directions(0), directions(1)
    mine = jnp.where(core == 0, even, odd).astype(BF16)
    other = jnp.where(core == 0, odd, even).astype(BF16)
    squares = line(0, 2 * tiles)
    squares = jnp.sum(jnp.sum(squares, axis=1, keepdims=True), axis=0, keepdims=True)
    rate = lax.rsqrt(squares / (RANK * KW) + 1e-06)
    both = jnp.concatenate([mine, other], axis=0)
    pieces = 4
    group = shards // pieces
    for piece in range(pieces):
        owners = slice(piece * group, piece * group + group)
        factor = jnp.concatenate(
            [
                sent_ref[owners, :rows, :].reshape(group * rows, half),
                swapped_ref[piece * group * rows : (piece + 1) * group * rows, :],
            ],
            axis=1,
        )
        step = dot32(factor, both) * (0.1 * rate)
        for i in range(cols // half):
            lanes = slice(i * half, i * half + half)
            old = old_ref[owners, :, i * share : i * share + share, :].astype(F32)
            copies_ref[owners, :, :, lanes] = (
                old - step[:, lanes].reshape(group, reps, share, half)
            ).astype(BF16)
    update = dot32(own_ref[...], both) * rate
    update_ref[...] = update
    weight_out_ref[...] = weight_ref[...] - 0.1 * update


def new_weights(gathered, sent, swapped, old, own_factor, weight):
    shards, reps = old.shape[:2]
    rows, cols = weight.shape
    return pl.pallas_call(
        new_weights_body,
        out_shape=(
            jax.ShapeDtypeStruct((shards, reps, rows // reps, cols), BF16),
            jax.ShapeDtypeStruct((rows, cols), F32),
            jax.ShapeDtypeStruct((rows, cols), F32),
        ),
        in_specs=6 * [VMEM_SPEC],
        out_specs=3 * (VMEM_SPEC,),
        cost_estimate=pl.CostEstimate(
            flops=4 * swapped.size * cols, bytes_accessed=8 * swapped.size, transcendentals=0
        ),
        compiler_params=pltpu.CompilerParams(vmem_limit_bytes=20 * MIB),
        name="new_weights",
    )(gathered, sent, swapped, old, own_factor, weight)


def on_device(
    tokens_in,
    query_two,
    key_two,
    values,
    out_grad,
    second_scale,
    factor,
    weight,
    first_moment,
    second_moment,
):
    shards = lax.axis_size("fs")
    reps = lax.axis_size("rep")
    rep = lax.axis_index("rep")
    half = factor.shape[1] // 2
    rows, cols = weight.shape
    tiles = cols // 128
    own_rows = first_moment.shape[0]
    pairs = own_rows // 2
    lines = own_rows * 2 * tiles

    message, own_factor = first_message(factor, weight, shards, reps)
    sent = lax.all_to_all(message, "fs", 0, 0, tiled=True)
    old_mine = sent[:, rows:]
    factor_mine = sent[:, :rows].reshape(-1, half)

    moments = lax.all_gather(jnp.concatenate([first_moment, second_moment], 0), "tp")
    moments = moments.reshape(2, 2, pairs, 2, tiles, 128)
    moments = moments.transpose(1, 3, 2, 0, 4, 5).reshape(2 * lines, 128)

    key_grad = key_gradient(query_two, key_two, values, out_grad, second_scale)
    key_both = lax.all_gather(key_grad, "tp", tiled=True)
    moments, key_both = lax.optimization_barrier((moments, key_both))

    sums = projected_sums(tokens_in, sent, key_both)
    arrived = lax.all_to_all(sums.reshape(shards, lines // 2, 128), "fs", 0, 0, tiled=True)
    part = lax.all_to_all(summed(arrived, 2 * reps), ("rep", "tp"), 0, 0, tiled=True)
    message, new_first, new_second = moments_step(
        part.reshape(reps * lines, 128), moments, shards
    )
    gathered = lax.all_to_all(message, "fs", 0, 0, tiled=True)

    old_all = jnp.zeros((shards, reps, *old_mine.shape[1:]), BF16)
    old_all = lax.dynamic_update_index_in_dim(old_all, old_mine, rep, 1)
    for i in (2, 1, 3):
        came = lax.ppermute(old_mine, "rep", [(j, (j + i) % reps) for j in range(reps)])
        old_all = lax.dynamic_update_index_in_dim(old_all, came, (rep + reps - i) % reps, 1)
    factor_other = lax.ppermute(factor_mine, "tp", [(0, 1), (1, 0)])

    copies, update_step, new_weight = new_weights(
        gathered, sent, factor_other, old_all, own_factor, weight
    )

    return (
        new_weight,
        copies.reshape(-1, cols),
        update_step,
        new_first,
        new_second,
    )


def solution(mesh):
    in_specs = (
        P(("fs", "rep"), None),
        P(("fs", "rep"), "tp"),
        P(("fs", "rep"), "tp"),
        P(("fs", "rep"), "tp"),
        P(("fs", "rep"), "tp"),
        P("tp"),
        P("fs", None),
        P("fs", "tp"),
        P("fs", "tp"),
        P("fs", "tp"),
    )
    out_specs = (P("fs", "tp"), P(None, "tp"), P("fs", "tp"), P("fs", "tp"), P("fs", "tp"))

    return jax.shard_map(
        on_device, mesh=mesh, in_specs=in_specs, out_specs=out_specs, check_vma=False
    )
```

```python
import jax
import jax.numpy as jnp
from jax import lax
from jax.experimental import pallas as pl
from jax.experimental.pallas import tpu as pltpu
from jax.sharding import PartitionSpec as P


RANK = 256
KW = 512
BF16 = jnp.bfloat16
F32 = jnp.float32

MIB = 1024 * 1024
VMEM_SPEC = pl.BlockSpec(memory_space=pltpu.VMEM)


def dot32(left, right):
    return jnp.dot(left, right, preferred_element_type=F32)


def dot_rows(left, right):
    return lax.dot_general(left, right, (((1,), (1,)), ((), ())), preferred_element_type=F32)


def key_gradient_body(scale_ref, query_ref, key_ref, value_ref, grad_ref, out_ref):
    length = query_ref.shape[0]
    block = length // 2
    heads = scale_ref.shape[0]
    dim = query_ref.shape[1] // heads
    wide = value_ref.shape[1] // heads
    inv_root = dim ** (-0.5)
    pair = 2 * dim
    lane = lax.broadcasted_iota(jnp.int32, (block, pair), 1)
    later = lax.broadcasted_iota(jnp.int32, (block, block), 0) > lax.broadcasted_iota(
        jnp.int32, (block, block), 1
    )
    for first in range(0, heads, 2):
        lanes = slice(first * dim, first * dim + pair)
        found = [[], []]
        for side in range(2):
            head = first + side
            span = slice(head * wide, head * wide + wide)
            for step in range(2):
                rows = slice(step * block, step * block + block)
                seen = block * (step + 1)
                own = query_ref[rows, lanes].astype(F32) * inv_root
                own = jnp.where((lane >= dim) == (side == 1), own, 0.0).astype(BF16)
                scores = dot_rows(key_ref[:seen, lanes], own)
                last = jnp.where(later, -1e30, scores[seen - block :])
                scores = jnp.concatenate([scores[: seen - block], last], axis=0) if step else last
                exps = jnp.exp(scores - jnp.max(scores, axis=0, keepdims=True))
                total = jnp.sum(exps, axis=0, keepdims=True)
                attn_grad = dot_rows(value_ref[:seen, span], grad_ref[rows, span])
                weights_map = exps / total
                inner = jnp.sum(weights_map * attn_grad, axis=0, keepdims=True)
                score_grad = (-scale_ref[head] * weights_map * (attn_grad - inner)).astype(BF16)
                for place in range(step + 1):
                    found[place].append(
                        dot32(score_grad[place * block : place * block + block], own)
                    )
        for place in range(2):
            total = found[place][0]
            for more in found[place][1:]:
                total = total + more
            out_ref[place * block : place * block + block, lanes] = total.astype(BF16)


def key_gradient(query_rows, key_rows, value_rows, grad_rows, second_scale):
    return pl.pallas_call(
        key_gradient_body,
        out_shape=jax.ShapeDtypeStruct(query_rows.shape, BF16),
        in_specs=[pl.BlockSpec(memory_space=pltpu.SMEM)] + 4 * [pl.BlockSpec(memory_space=pltpu.VMEM)],
        out_specs=pl.BlockSpec(memory_space=pltpu.VMEM),
        compiler_params=pltpu.CompilerParams(vmem_limit_bytes=24 * MIB),
        name="key_gradient",
    )(second_scale, query_rows, key_rows, value_rows, grad_rows)


def first_message_body(
    factor_hbm, weight_hbm, out_hbm, own_ref, factor_ref, weight_ref, out_ref, sems
):
    shards = out_ref.shape[0]
    rows, rank = factor_ref.shape
    half = rank // 2
    share = weight_ref.shape[0]
    start = pl.multiple_of(lax.axis_index("rep") * share, share)
    factor_copy = pltpu.make_async_copy(factor_hbm, factor_ref, sems.at[0])
    weight_copy = pltpu.make_async_copy(weight_hbm.at[pl.ds(start, share), :], weight_ref, sems.at[1])
    factor_copy.start()
    weight_copy.start()
    core = lax.axis_index("tp")
    ranks = lax.broadcasted_iota(jnp.int32, (rank, half), 0)
    places = lax.broadcasted_iota(jnp.int32, (rank, half), 1)
    pair = sum((places >= i * shards).astype(jnp.int32) for i in range(1, half // shards))
    wanted = (places - pair * shards) * (rank // shards) + 2 * pair
    pick = (ranks == wanted + core).astype(F32).astype(BF16)
    pick_other = (ranks == wanted + 1 - core).astype(F32).astype(BF16)
    factor_copy.wait()
    factor = factor_ref[...]
    mine = dot32(factor, pick).astype(BF16)
    own_ref[:, :half] = mine
    out_ref[:, :rows, :] = jnp.broadcast_to(mine[None], (shards, rows, half))
    weight_copy.wait()
    old = weight_ref[...].astype(BF16)
    for i in range(2):
        piece = old[:, i * half : i * half + half]
        out_ref[:, rows + i * share : rows + i * share + share, :] = jnp.broadcast_to(
            piece[None], (shards, share, half)
        )
    out_copy = pltpu.make_async_copy(out_ref, out_hbm, sems.at[0])
    out_copy.start()
    own_ref[:, half:] = dot32(factor, pick_other).astype(BF16)
    out_copy.wait()


def first_message(factor, weight, shards, reps):
    rows, rank = factor.shape
    half = rank // 2
    share = rows // reps
    message = (shards, rows + 2 * share, half)
    any_spec = pl.BlockSpec(memory_space=pltpu.HBM)
    return pl.pallas_call(
        first_message_body,
        out_shape=(
            jax.ShapeDtypeStruct(message, BF16),
            jax.ShapeDtypeStruct((rows, rank), BF16),
        ),
        in_specs=2 * [any_spec],
        out_specs=(any_spec, VMEM_SPEC),
        scratch_shapes=[
            pltpu.VMEM((rows, rank), BF16),
            pltpu.VMEM((share, weight.shape[1]), F32),
            pltpu.VMEM(message, BF16),
            pltpu.SemaphoreType.DMA((2,)),
        ],
        compiler_params=pltpu.CompilerParams(vmem_limit_bytes=60 * MIB),
        name="first_message",
    )(factor, weight)


def projected_sums_body(tokens_ref, sent_ref, grad_ref, out_ref, old_hbm, laid_ref, sem):
    shards, _, half = sent_ref.shape
    length, width = tokens_ref.shape
    rows = width // shards
    old_copy = pltpu.make_async_copy(sent_ref.at[:, rows:, :], old_hbm, sem)
    old_copy.start()
    cols = grad_ref.shape[1]
    pairs = half // shards
    factor = sent_ref[:, :rows, :].reshape(width, half)
    reduced = dot32(tokens_ref[...], factor).T
    high = reduced.astype(BF16)
    low = (reduced - high.astype(F32)).astype(BF16)
    tiles = cols // 128
    for i in range(2):
        grads = grad_ref[i * length : i * length + length, :]
        sums = dot32(high, grads) + dot32(low, grads)
        for pair in range(pairs):
            for tile in range(tiles):
                place = (pair * 2 + i) * tiles + tile
                laid_ref[pl.ds(place, shards, 2 * pairs * tiles), :] = sums[
                    pair * shards : pair * shards + shards, tile * 128 : tile * 128 + 128
                ]
    out_ref[...] = laid_ref[...].astype(BF16)
    old_copy.wait()


def projected_sums(tokens, sent, grads):
    shards, sent_rows, half = sent.shape
    total = half * 2 * grads.shape[1] // 128
    old = (shards, sent_rows - tokens.shape[1] // shards, half)
    return pl.pallas_call(
        projected_sums_body,
        out_shape=(jax.ShapeDtypeStruct((total, 128), BF16), pltpu.HBM(old, BF16)),
        in_specs=3 * [VMEM_SPEC],
        out_specs=(VMEM_SPEC, pl.BlockSpec(memory_space=pltpu.HBM)),
        scratch_shapes=[pltpu.VMEM((total, 128), F32), pltpu.SemaphoreType.DMA],
        cost_estimate=pl.CostEstimate(
            flops=4 * tokens.size * half, bytes_accessed=2 * tokens.size, transcendentals=0
        ),
        compiler_params=pltpu.CompilerParams(vmem_limit_bytes=16 * MIB),
        name="projected_sums",
    )(tokens, sent, grads)


def summed_body(arrived_ref, out_ref):
    total = jnp.sum(arrived_ref[...].astype(F32), axis=0)
    out_ref[...] = jnp.broadcast_to(total[None], out_ref.shape)


def summed(arrived, count):
    return pl.pallas_call(
        summed_body,
        out_shape=jax.ShapeDtypeStruct((count, *arrived.shape[1:]), F32),
        in_specs=[VMEM_SPEC],
        out_specs=VMEM_SPEC,
        compiler_params=pltpu.CompilerParams(vmem_limit_bytes=4 * MIB),
        name="summed",
    )(arrived)


def moments_step_body(part_ref, moments_ref, message_ref, first_ref, second_ref):
    lines = moments_ref.shape[0] // 2
    core = lax.axis_index("tp")
    total = part_ref[:lines, :]
    for i in range(lines, part_ref.shape[0], lines):
        total = total + part_ref[i : i + lines, :]
    new_first = 0.9 * moments_ref[:lines, :] + 0.1 * total
    new_second = 0.95 * moments_ref[lines:, :] + 0.05 * total * total
    direction = (new_first / (jnp.sqrt(new_second) + 1e-08)).astype(BF16).astype(F32)
    squares = direction * direction
    squares = jnp.sum(jnp.sum(squares, axis=1, keepdims=True), axis=0, keepdims=True)
    tiles = lines // 8

    def own_row(value, pair, parity):
        base = (parity * 2 + pair) * 2 * tiles
        return jnp.concatenate(
            [
                jnp.where(
                    core == 0,
                    value[base + tile : base + tile + 1],
                    value[base + tiles + tile : base + tiles + tile + 1],
                )
                for tile in range(tiles)
            ],
            axis=1,
        )

    for pair in range(2):
        for parity in range(2):
            row = pair * 2 + parity
            first_ref[row : row + 1, :] = own_row(new_first, pair, parity)
            second_ref[row : row + 1, :] = own_row(new_second, pair, parity)
    own = [
        jnp.concatenate([own_row(direction, pair, parity) for parity in range(2)], axis=1)
        for pair in range(2)
    ]
    high = squares.astype(BF16).astype(F32)
    middle = (squares - high).astype(BF16).astype(F32)
    low = squares - high - middle
    lane = lax.broadcasted_iota(jnp.int32, (1, 128), 1)
    packed = jnp.where(lane == 0, high, jnp.where(lane == 1, middle, jnp.where(lane == 2, low, 0.0)))
    own[0] = jnp.concatenate([own[0], packed], axis=1)
    own[1] = jnp.concatenate([own[1], jnp.zeros_like(packed)], axis=1)
    message = jnp.concatenate(own, axis=0).astype(BF16)
    message_ref[...] = jnp.broadcast_to(message[None], message_ref.shape)


def moments_step(part, moments, shards):
    lines = moments.shape[0] // 2
    return pl.pallas_call(
        moments_step_body,
        out_shape=(
            jax.ShapeDtypeStruct((shards, 2, lines * 32 + 128), BF16),
            jax.ShapeDtypeStruct((4, lines * 16), F32),
            jax.ShapeDtypeStruct((4, lines * 16), F32),
        ),
        in_specs=2 * [VMEM_SPEC],
        out_specs=3 * (VMEM_SPEC,),
        compiler_params=pltpu.CompilerParams(vmem_limit_bytes=4 * MIB),
        name="moments_step",
    )(part, moments)


def new_weights_body(
    gathered_ref, sent_ref, swapped_ref, old_ref, own_ref, weight_ref,
    copies_ref, update_ref, weight_out_ref,
):
    shards = sent_ref.shape[0]
    width, half = swapped_ref.shape
    rows = width // shards
    reps, share = copies_ref.shape[1:3]
    cols = weight_ref.shape[1]
    tiles = cols // 128
    pairs = half // shards
    core = lax.axis_index("tp")

    def line(pair, place):
        return gathered_ref[:, pair, place * 128 : place * 128 + 128].astype(F32)

    def directions(parity):
        return jnp.concatenate(
            [
                jnp.concatenate(
                    [line(pair, parity * tiles + tile) for tile in range(tiles)], axis=1
                )
                for pair in range(pairs)
            ],
            axis=0,
        )

    even, odd = directions(0), directions(1)
    mine = jnp.where(core == 0, even, odd).astype(BF16)
    other = jnp.where(core == 0, odd, even).astype(BF16)
    squares = line(0, 2 * tiles)
    squares = jnp.sum(jnp.sum(squares, axis=1, keepdims=True), axis=0, keepdims=True)
    rate = lax.rsqrt(squares / (RANK * KW) + 1e-06)
    both = jnp.concatenate([mine, other], axis=0)
    pieces = 4
    group = shards // pieces
    for piece in range(pieces):
        owners = slice(piece * group, piece * group + group)
        factor = jnp.concatenate(
            [
                sent_ref[owners, :rows, :].reshape(group * rows, half),
                swapped_ref[piece * group * rows : (piece + 1) * group * rows, :],
            ],
            axis=1,
        )
        step = dot32(factor, both) * (0.1 * rate)
        for i in range(cols // half):
            lanes = slice(i * half, i * half + half)
            old = old_ref[owners, :, i * share : i * share + share, :].astype(F32)
            copies_ref[owners, :, :, lanes] = (
                old - step[:, lanes].reshape(group, reps, share, half)
            ).astype(BF16)
    update = dot32(own_ref[...], both) * rate
    update_ref[...] = update
    weight_out_ref[...] = weight_ref[...] - 0.1 * update


def new_weights(gathered, sent, swapped, old, own_factor, weight):
    shards, reps = old.shape[:2]
    rows, cols = weight.shape
    return pl.pallas_call(
        new_weights_body,
        out_shape=(
            jax.ShapeDtypeStruct((shards, reps, rows // reps, cols), BF16),
            jax.ShapeDtypeStruct((rows, cols), F32),
            jax.ShapeDtypeStruct((rows, cols), F32),
        ),
        in_specs=6 * [VMEM_SPEC],
        out_specs=3 * (VMEM_SPEC,),
        cost_estimate=pl.CostEstimate(
            flops=4 * swapped.size * cols, bytes_accessed=8 * swapped.size, transcendentals=0
        ),
        compiler_params=pltpu.CompilerParams(vmem_limit_bytes=20 * MIB),
        name="new_weights",
    )(gathered, sent, swapped, old, own_factor, weight)


def on_device(
    tokens_in,
    query_two,
    key_two,
    values,
    out_grad,
    second_scale,
    factor,
    weight,
    first_moment,
    second_moment,
):
    shards = lax.axis_size("fs")
    reps = lax.axis_size("rep")
    rep = lax.axis_index("rep")
    half = factor.shape[1] // 2
    rows, cols = weight.shape
    tiles = cols // 128
    own_rows = first_moment.shape[0]
    pairs = own_rows // 2
    lines = own_rows * 2 * tiles

    message, own_factor = first_message(factor, weight, shards, reps)
    sent = lax.all_to_all(message, "fs", 0, 0, tiled=True)
    factor_mine = sent[:, :rows].reshape(-1, half)

    moments = lax.all_gather(jnp.concatenate([first_moment, second_moment], 0), "tp")
    moments = moments.reshape(2, 2, pairs, 2, tiles, 128)
    moments = moments.transpose(1, 3, 2, 0, 4, 5).reshape(2 * lines, 128)

    key_grad = key_gradient(query_two, key_two, values, out_grad, second_scale)
    key_both = lax.all_gather(key_grad, "tp", tiled=True)
    moments, key_both = lax.optimization_barrier((moments, key_both))

    sums, old_mine = projected_sums(tokens_in, sent, key_both)
    arrived = lax.all_to_all(sums.reshape(shards, lines // 2, 128), "fs", 0, 0, tiled=True)
    part = lax.all_to_all(summed(arrived, 2 * reps), ("rep", "tp"), 0, 0, tiled=True)
    message, new_first, new_second = moments_step(
        part.reshape(reps * lines, 128), moments, shards
    )
    gathered = lax.all_to_all(message, "fs", 0, 0, tiled=True)

    old_all = jnp.zeros((shards, reps, *old_mine.shape[1:]), BF16)
    old_all = lax.dynamic_update_index_in_dim(old_all, old_mine, rep, 1)
    for i in (2, 1, 3):
        came = lax.ppermute(old_mine, "rep", [(j, (j + i) % reps) for j in range(reps)])
        old_all = lax.dynamic_update_index_in_dim(old_all, came, (rep + reps - i) % reps, 1)
    factor_other = lax.ppermute(factor_mine, "tp", [(0, 1), (1, 0)])

    copies, update_step, new_weight = new_weights(
        gathered, sent, factor_other, old_all, own_factor, weight
    )

    return (
        new_weight,
        copies.reshape(-1, cols),
        update_step,
        new_first,
        new_second,
    )


def solution(mesh):
    in_specs = (
        P(("fs", "rep"), None),
        P(("fs", "rep"), "tp"),
        P(("fs", "rep"), "tp"),
        P(("fs", "rep"), "tp"),
        P(("fs", "rep"), "tp"),
        P("tp"),
        P("fs", None),
        P("fs", "tp"),
        P("fs", "tp"),
        P("fs", "tp"),
    )
    out_specs = (P("fs", "tp"), P(None, "tp"), P("fs", "tp"), P("fs", "tp"), P("fs", "tp"))

    return jax.shard_map(
        on_device, mesh=mesh, in_specs=in_specs, out_specs=out_specs, check_vma=False
    )
```
